32 devices in a mesh: grp: 2 (over y), sp: 4 (over z), tp: 4 (over x, core).
Axes of the slice: x: 2, y: 2, z: 4, core: 2. Of those that a mesh axis runs over, the one named last changes fastest.
Arguments:
- queries: bfloat16 [2048, 512], P(('grp', 'sp'), 'tp'), parts along dimension 0, may hold values from -6 to 6
- key_rows: bfloat16 [2048, 512], P(('grp', 'sp'), 'tp'), parts along dimension 0, may hold values from -6 to 6
- value_rows: bfloat16 [2048, 1024], P(('grp', 'sp'), 'tp'), parts along dimension 0, may hold values from -6 to 6
- out_gate: bfloat16 [2048, 1024], P(('grp', 'sp'), 'tp'), parts along dimension 0, may hold values from -6 to 6
- log_decay: float32 [2, 2048, 512], P(None, ('grp', 'sp'), 'tp'), parts along dimension 1
- doc_ids: int32 [2048], P(('grp', 'sp')), parts along dimension 0, may hold values from 0 to 1, as said below
- head_gain: float32 [1024], P('tp'), may hold values from 0.1 to 1.9
- out_weight: bfloat16 [1024, 2048], P('tp'), may hold values from -0.375 to 0.375
- residual: bfloat16 [2048, 2048], P(('grp', 'sp'), 'tp'), parts along dimension 0
- norm_gain: float32 [2, 2048], replicated, may hold values from 0.1 to 1.9
- norm_bias: float32 [2, 2048], replicated, may hold values from -3 to 3
- gate_weight: bfloat16 [2048, 3072], P('sp', 'tp'), may hold values from -0.125 to 0.125
- up_weight: bfloat16 [2048, 3072], P('sp', 'tp'), may hold values from -0.125 to 0.125
- down_weight: bfloat16 [3072, 2048], P('tp', 'sp'), may hold values from -0.109375 to 0.109375
Outputs:
- layer_out: bfloat16 [2048, 2048], P(('grp', 'sp'), 'tp'), parts along dimension 0
The draws below stay inside these ranges and needn't reach their ends.
There are 2 independent parts, one for each index of `grp`. The reference program is written for one: setup_inputs(seed, part) draws one part's arguments, and reference() takes and returns one part's arrays. A program takes and returns all parts, laid end to end along the dimension named above; an argument that names none is the same for every part. Nothing has to cross between parts.
Inputs may be any that keep to these rules, and one draw needn't show every extreme that they name: `doc_ids`: document numbers start at 0 and never fall; they rise by one at each of 1 positions, the k-th rise lying within half of 256 positions of k times 1024 divided by 2.
All inputs are finite; a program needn't handle non-finite values.
Results may differ from the reference program's by a relative error of at most 0.009.
Values may be sent and summed in bfloat16 or wider, within the bound.
A program may use at most 128 MiB of HBM per device.

```python
import math
import jax
import jax.numpy as jnp
from jax import lax

D = 2048
HEADS = 16
DK = 32
DV = 64
FF = 3072
BLOCK = 64
TOK_DEV = 256
SEQ = 1024
DOCS = 2
KW = 512
GW = 1024
N_TP = 4


def draw_log_decay(key, part):
    streams = jax.random.split(key, 6)
    fast_share = 0.5
    fast = jax.random.uniform(streams[0], (2, 1, KW)) < fast_share
    decay_speed = jnp.where(fast, 1.0 / 40.0, 0.5 * DOCS / SEQ)
    reach_multiplier = jnp.exp(jax.random.uniform(streams[1], (2, SEQ // TOK_DEV, 1), minval=-0.9, maxval=0.9))
    reach_multiplier = jnp.repeat(reach_multiplier, TOK_DEV, axis=1)
    block_multiplier = jnp.exp(jax.random.uniform(streams[2], (2, SEQ // BLOCK, 1), minval=-0.35, maxval=0.35))
    block_multiplier = jnp.repeat(block_multiplier, BLOCK, axis=1)
    random_perturbation = jnp.exp(0.5 * jax.random.normal(streams[3], (2, SEQ, KW)))
    marked_locations = jax.random.randint(streams[4], (2, 8, 1), 0, SEQ)
    layer_depth_count = jnp.log(jax.random.uniform(streams[5], (2, 8, 1), minval=0.5, maxval=0.8))
    token_location = jnp.arange(SEQ, dtype=jnp.int32)[None, None, :]
    spike_amplitude = jnp.sum(jnp.where(marked_locations == token_location, layer_depth_count, 0.0), axis=1)
    return (-decay_speed * reach_multiplier * block_multiplier * random_perturbation + spike_amplitude[:, :, None]).astype(jnp.float32)


def draw_doc_ids(key, part):
    shifts = jax.random.randint(key, (DOCS - 1,), -(TOK_DEV // 2), TOK_DEV // 2 + 1)
    cuts = jnp.arange(1, DOCS, dtype=jnp.int32) * (SEQ // DOCS) + shifts
    token_location = jnp.arange(SEQ, dtype=jnp.int32)
    return jnp.sum((token_location[:, None] >= cuts[None, :]).astype(jnp.int32), axis=1)


def draw_residual(key, part):
    streams = jax.random.split(key, 3)
    base = jax.random.normal(streams[0], (SEQ, D))
    rising = 3.0 ** (jnp.arange(D, dtype=jnp.float32) / (D - 1))
    rising = rising * jnp.exp(jax.random.uniform(streams[1], (D,), minval=-0.4, maxval=0.4))
    row_scale = jnp.exp(jax.random.uniform(streams[2], (SEQ, 1), minval=math.log(0.5), maxval=math.log(5.0)))
    return (base * rising * row_scale).astype(jnp.bfloat16)


def steps_of(stream_key, shape, cuts, least, high):
    def one(position, parts):
        steps = jax.random.uniform(jax.random.fold_in(jax.random.fold_in(stream_key, 6), position), (parts,), jnp.float32, least / len(cuts), high / len(cuts))
        return jnp.repeat(jnp.exp(steps), shape[position] // parts).reshape((-1,) + (1,) * (len(shape) - position - 1))

    factor_of = one(*cuts[0])
    for cut in cuts[1:]:
        factor_of = factor_of * one(*cut)
    return factor_of


def bell_draw(own_key, shape, width, reach, pieces=(), kind=jnp.bfloat16):
    loudness = steps_of(own_key, shape, pieces, -0.22, 0.18) if pieces else 1.0
    drawn = jax.random.normal(own_key, shape, jnp.float32) * width * loudness
    return jnp.minimum(jnp.maximum(drawn, -reach), reach).astype(kind)


def setup_inputs(seed: int = 0, part: int = 0) -> dict:
    key_list = jax.random.split(jax.random.key(seed), 15)
    part_splits = jax.random.split(jax.random.fold_in(key_list[14], part), 15)
    return {
        "queries": bell_draw(part_splits[0], (SEQ, KW), 1.0, 6.0, ((0, 4), (1, 4))),
        "key_rows": bell_draw(part_splits[1], (SEQ, KW), 1.0, 6.0, ((0, 4), (1, 4))),
        "value_rows": bell_draw(part_splits[2], (SEQ, GW), 1.0, 6.0, ((0, 4), (1, 4))),
        "out_gate": bell_draw(part_splits[3], (SEQ, GW), 1.0, 6.0, ((0, 4), (1, 4))),
        "log_decay": draw_log_decay(jax.random.fold_in(jax.random.fold_in(key_list[14], part), 71), part),
        "doc_ids": draw_doc_ids(jax.random.fold_in(jax.random.fold_in(key_list[14], part), 71), part),
        "head_gain": jnp.clip(1.0 + 0.18 * jax.random.normal(key_list[6], (GW,), jnp.float32), 0.1, 1.9),
        "out_weight": bell_draw(key_list[7], (GW, D), (GW // 4) ** -0.5, 0.375, ((0, 4),)),
        "residual": draw_residual(jax.random.fold_in(jax.random.fold_in(key_list[14], part), 71), part),
        "norm_gain": jnp.clip(1.0 + 0.18 * jax.random.normal(key_list[9], (2, D), jnp.float32), 0.1, 1.9),
        "norm_bias": bell_draw(key_list[10], (2, D), 0.5, 3.0, (), jnp.float32),
        "gate_weight": bell_draw(key_list[11], (D, FF), D ** -0.5, 0.125, ((0, 4), (1, 4))),
        "up_weight": bell_draw(key_list[12], (D, FF), D ** -0.5, 0.125, ((0, 4), (1, 4))),
        "down_weight": bell_draw(key_list[13], (FF, D), FF ** -0.5, 0.109375, ((0, 4), (1, 4))),
    }


EPS = 1e-06
HIGH = lax.Precision.HIGHEST

def run_blocks(query, key_part, value_part, decay, docs):
    length = query.shape[0]
    count = length // BLOCK
    head_count = query.shape[1]
    lower = jnp.arange(BLOCK)[:, None] >= jnp.arange(BLOCK)[None, :]

    def blocked(array):
        return array.reshape((count, BLOCK) + array.shape[1:])

    def advance(carried, inputs):
        state, state_doc = carried
        query_block, key_block, value_block, decay_block, doc_block = inputs
        running = jnp.cumsum(decay_block, axis=0)
        allowed = lower & (doc_block[:, None] == doc_block[None, :])
        relative = jnp.exp(jnp.where(allowed[:, :, None, None], running[:, None] - running[None, :], -jnp.inf))
        scores = jnp.einsum('ihd,jhd,ijhd->hij', query_block, key_block, relative, precision=HIGH)
        within = jnp.einsum('hij,jhe->ihe', scores, value_block, precision=HIGH)
        linked = (doc_block == state_doc).astype(query.dtype)
        carried_part = jnp.einsum('ihd,hde->ihe', query_block * jnp.exp(running), state, precision=HIGH) * linked[:, None, None]
        closing = doc_block[-1]
        ending = (doc_block == closing).astype(query.dtype)
        tail_decay = jnp.exp(running[-1][None] - running) * ending[:, None, None]
        kept = (state_doc == closing).astype(query.dtype)
        state = kept * jnp.exp(running[-1])[:, :, None] * state + jnp.einsum('jhd,jhe->hde', key_block * tail_decay, value_block, precision=HIGH)
        return ((state, closing), within + carried_part)
    start = (jnp.zeros((head_count, query.shape[2], value_part.shape[2]), jnp.float32), jnp.array(-1, jnp.int32))
    (state, closing), outputs = lax.scan(advance, start, tuple((blocked(array) for array in (query, key_part, value_part, decay, docs))))
    return (outputs.reshape(length, head_count, value_part.shape[2]), state, closing)

def layer_norm(stream, gain, bias):
    middle = lax.optimization_barrier(jnp.mean(stream, axis=-1, keepdims=True))
    spread = lax.optimization_barrier(jnp.mean(jnp.square(stream - middle), axis=-1, keepdims=True))
    return (stream - middle) * lax.rsqrt(spread + EPS) * gain + bias

def group_sum(left, right):
    group_width = left.shape[1] // N_TP
    summed = jnp.zeros((left.shape[0], right.shape[1]), jnp.float32)
    for group in range(N_TP):
        term = jnp.dot(left[:, group * group_width:(group + 1) * group_width], right[group * group_width:(group + 1) * group_width], preferred_element_type=jnp.float32)
        summed = summed + lax.optimization_barrier(term.astype(jnp.bfloat16)).astype(jnp.float32)
    return summed

def reference(queries, key_rows, value_rows, out_gate, log_decay, doc_ids, head_gain, out_weight, residual, norm_gain, norm_bias, gate_weight, up_weight, down_weight):
    length = queries.shape[0]
    query = queries.astype(jnp.float32).reshape(length, HEADS, DK) * DK ** (-0.5)
    key_part = key_rows.astype(jnp.float32).reshape(length, HEADS, DK)
    value_part = value_rows.astype(jnp.float32).reshape(length, HEADS, DV)
    forward_decay = log_decay[0].reshape(length, HEADS, DK)
    backward_decay = log_decay[1].reshape(length, HEADS, DK)
    forward_out = run_blocks(query, key_part, value_part, forward_decay, doc_ids)[0]
    backward_out = run_blocks(query[::-1], key_part[::-1], value_part[::-1], backward_decay[::-1], doc_ids[::-1])[0][::-1]
    attended = forward_out + backward_out
    normed = attended * lax.rsqrt(lax.optimization_barrier(jnp.mean(attended * attended, axis=-1, keepdims=True)) + EPS)
    mixed = (normed.reshape(length, GW) * head_gain * jax.nn.silu(out_gate.astype(jnp.float32))).astype(jnp.bfloat16)
    branch = group_sum(mixed, out_weight)
    settled = layer_norm(residual.astype(jnp.float32) + branch, norm_gain[0], norm_bias[0])
    features = settled.astype(jnp.bfloat16)
    gate = jnp.dot(features, gate_weight, preferred_element_type=jnp.float32)
    up_part = jnp.dot(features, up_weight, preferred_element_type=jnp.float32)
    inner = (jax.nn.silu(gate) * up_part).astype(jnp.bfloat16)
    down = group_sum(inner, down_weight)
    return layer_norm(settled + 0.5 * down, norm_gain[1], norm_bias[1]).astype(jnp.bfloat16)
```

```python
import functools

import jax
import jax.numpy as jnp
from jax import lax
from jax.experimental import pallas as pl
from jax.experimental.pallas import tpu as pltpu
from jax.sharding import PartitionSpec as P

DK = 32
DV = 64
EPS = 1e-06
F32 = jnp.float32
BF16 = jnp.bfloat16
HIGH = lax.Precision.HIGHEST
MESH = pl.DeviceIdType.MESH
VMEM = pltpu.VMEM


def dot(a, b, dims=((1,), (0,)), precision=None):
    return lax.dot_general(a, b, (dims, ((), ())), precision=precision, preferred_element_type=F32)


def iota(shape, axis):
    return lax.broadcasted_iota(jnp.int32, shape, axis)


def attend_kernel(q_ref, k_ref, v_ref, decay_ref, doc_ref, docrow_ref, out_ref, qf_ref, qb_ref, state_ref, aux_ref, acc):
    length, width = q_ref.shape
    heads = width // DK
    q = q_ref[...].astype(F32) * DK**-0.5
    k = k_ref[...].astype(F32)
    v = v_ref[...]
    row = iota((length, width), 0)
    far = iota((length, length), 0) ^ iota((length, length), 1)
    lane_head = (iota((length, 2 * width), 1) % width) // DK
    zero = jnp.zeros((length, width), F32)

    def scores(left, right):
        left, right = left.astype(BF16), right.astype(BF16)
        lanes = lane_head[:, : left.shape[1]]
        stacked = jnp.concatenate([jnp.where(lanes == h, left, jnp.zeros_like(left)) for h in range(heads)], axis=0)
        return dot(stacked, right, ((1,), (1,)))

    acc[...] = 2.0 * scores(q, k)
    total_f, total_b = decay_ref[0], decay_ref[1]
    prefix_f, suffix_b = total_f, total_b
    suffix_f, prefix_b = zero, zero
    span = 1
    while span < length:
        upper = (row & span) != 0
        left = jnp.concatenate(
            [jnp.where(upper, q * jnp.exp(prefix_f), 0.0), jnp.where(upper, 0.0, q * jnp.exp(suffix_b))], axis=1
        )
        right = jnp.concatenate(
            [jnp.where(upper, 0.0, k * jnp.exp(suffix_f)), jnp.where(upper, k * jnp.exp(prefix_b), 0.0)], axis=1
        )
        product = scores(left, right)
        for h in range(heads):
            rows = slice(h * length, (h + 1) * length)
            acc[rows] = jnp.where(far >= span, product[rows], acc[rows])

        def other(x):
            return jnp.where(upper, pltpu.roll(x, span, 0), pltpu.roll(x, length - span, 0))

        beside_f, beside_b = other(total_f), other(total_b)
        prefix_f = prefix_f + jnp.where(upper, beside_f, 0.0)
        suffix_f = suffix_f + jnp.where(upper, 0.0, beside_f)
        suffix_b = suffix_b + jnp.where(upper, 0.0, beside_b)
        prefix_b = prefix_b + jnp.where(upper, beside_b, 0.0)
        total_f, total_b = total_f + beside_f, total_b + beside_b
        span *= 2

    doc = doc_ref[...]
    same = doc == docrow_ref[...]
    value_head = iota((length, v.shape[1]), 1) // DV
    result = jnp.zeros((length, v.shape[1]), F32)
    for h in range(heads):
        weights = jnp.where(same, acc[h * length : (h + 1) * length], 0.0).astype(BF16)
        result = jnp.where(value_head == h, dot(weights, v), result)
    out_ref[...] = result
    qf_ref[...] = q * jnp.exp(prefix_f)
    qb_ref[...] = q * jnp.exp(suffix_b)

    first, last = doc[:1], doc[length - 1 :]
    own = (iota((width, v.shape[1]), 0) // DK) == (iota((width, v.shape[1]), 1) // DV)
    for i, (reach, edge) in enumerate(((suffix_f, last), (prefix_b, first))):
        kept = jnp.where(doc == edge, k * jnp.exp(reach), 0.0).astype(BF16)
        state = jnp.where(own, dot(kept, v, ((0,), (0,))), 0.0)
        packed = state[:DK]
        for h in range(1, heads):
            packed = packed + state[h * DK : (h + 1) * DK]
        state_ref[i * DK : (i + 1) * DK] = packed.astype(BF16)
    edge_row = iota((8, width), 0)
    aux = jnp.where(edge_row == 0, jnp.exp(total_f[:8]), jnp.exp(total_b[:8]))
    aux = jnp.where(edge_row == 2, first, aux)
    aux_ref[...] = jnp.where(edge_row == 3, last, aux)


def layer_kernel(
    sizes,
    local_ref,
    qf_ref,
    qb_ref,
    state_ref,
    aux_ref,
    doc_ref,
    outgate_ref,
    headgain_ref,
    outweight_ref,
    residual_ref,
    gain_ref,
    bias_ref,
    gate_hbm,
    up_hbm,
    down_hbm,
    result_ref,
    gate_all,
    up_all,
    down_all,
    states,
    auxes,
    sendbuf,
    landed,
    sendbuf2,
    landed2,
    features,
    moments,
    moments_in,
    small_send,
    small_recv,
    z_send,
    z_recv,
    y_send,
    y_recv,
    tp_send,
    tp_recv,
    local_sem,
):
    n_grp, n_sp, n_tp = sizes
    g, s, t = lax.axis_index("grp"), lax.axis_index("sp"), lax.axis_index("tp")
    length = local_ref.shape[0]
    own_width = residual_ref.shape[1]
    full_width = own_width * n_tp

    def around(axis, me, n, d):
        return {axis: lax.rem(me + d, n)}

    barrier = pltpu.get_barrier_semaphore()
    for axis, me, n in (("grp", g, n_grp), ("sp", s, n_sp), ("tp", t, n_tp)):
        for d in range(1, n):
            pl.semaphore_signal(barrier, inc=1, device_id=around(axis, me, n, d), device_id_type=MESH)
    pl.semaphore_wait(barrier, n_grp + n_sp + n_tp - 3)

    sent = []

    def remote(src, dst, ssem, rsem, to):
        return pltpu.make_async_remote_copy(
            src_ref=src, dst_ref=dst, send_sem=ssem, recv_sem=rsem, device_id=to, device_id_type=MESH
        )

    small = []
    for d in range(1, n_sp):
        to = around("sp", s, n_sp, d)
        for j, (src, dst) in enumerate(((state_ref, states), (aux_ref, auxes))):
            copy = remote(src, dst.at[d - 1], small_send.at[j, d - 1], small_recv.at[j, d - 1], to)
            copy.start()
            small.append(copy)

    whole = ((gate_hbm, gate_all), (up_hbm, up_all), (down_hbm, down_all))

    def part(p, origin, which):
        src, dst = whole[p]
        rows = src.shape[0] // n_grp
        return dst.at[origin, pl.ds(pl.multiple_of(which * rows, rows), rows), :]

    def own_part(p):
        src, _ = whole[p]
        rows = src.shape[0] // n_grp
        return src.at[pl.ds(pl.multiple_of(g * rows, rows), rows), :]

    def along(p, way, k, origin):
        step = 1 if way == 0 else -1
        src = own_part(p) if k == 0 else part(p, origin, g)
        return remote(
            src, part(p, origin, g), z_send.at[p, way, k], z_recv.at[p, way, k], {"sp": lax.rem(s + step + n_sp, n_sp)}
        )

    def across(p, way, k, origin, d):
        return remote(
            part(p, origin, g), part(p, origin, g), y_send.at[p, way, k, d - 1], y_recv.at[p, way, k, d - 1],
            around("grp", g, n_grp, d),
        )

    def inside(x):
        return (x >= 0) & (x < n_sp)

    for p in range(3):
        for way in range(2):
            step = 1 if way == 0 else -1

            @pl.when(inside(s + step))
            def _(p=p, way=way):
                along(p, way, 0, s).start()

    own_copies = []
    for p in range(3):
        copy = pltpu.make_async_copy(whole[p][0], whole[p][1].at[s], local_sem.at[p])
        copy.start()
        own_copies.append(copy)

    def relay(k, p):
        for way in range(2):
            step = 1 if way == 0 else -1
            origin = s - step * k

            @pl.when(inside(origin))
            def _(way=way, step=step, origin=origin):
                along(p, way, k - 1, origin).wait_recv()
                if k < n_sp - 1:

                    @pl.when(inside(s + step))
                    def _():
                        along(p, way, k, origin).start()

                for d in range(1, n_grp):
                    across(p, way, k, origin, d).start()

    def finish_across(k, p):
        for way in range(2):
            origin = s - (1 if way == 0 else -1) * k

            @pl.when(inside(origin))
            def _(way=way, origin=origin):
                for d in range(1, n_grp):
                    arrived = part(p, origin, lax.rem(g - d + n_grp, n_grp))
                    sems = (y_send.at[p, way, k, d - 1], y_recv.at[p, way, k, d - 1])
                    remote(arrived, arrived, *sems, around("grp", g, n_grp, d)).wait_recv()

    events = [(k, p) for k in range(1, n_sp) for p in range(3)]
    cursor = [0]

    def pump(count):
        for k, p in events[cursor[0] : cursor[0] + count]:
            relay(k, p)
        cursor[0] += count

    def to_tp(kind, src_of, dst_of):
        copies = []
        for d in range(1, n_tp):
            to = lax.rem(t + d, n_tp)
            copy = remote(
                src_of(to), dst_of(d), tp_send.at[kind, d - 1], tp_recv.at[kind, d - 1], {"tp": to}
            )
            copy.start()
            copies.append(copy)
        sent.extend(copies)
        return copies

    for copy in small:
        copy.wait_recv()
    sent.extend(small)
    doc = doc_ref[...]
    first, last = doc[:1], doc[length - 1 :]
    width = qf_ref.shape[1]
    heads = width // DK
    value_width = local_ref.shape[1]
    own = (iota((width, value_width), 0) // DK) == (iota((width, value_width), 1) // DV)
    attended = local_ref[...]
    for back in range(2):
        query = (qb_ref if back else qf_ref)[...]
        edge = last if back else first
        reach = jnp.ones((1, width), F32)
        entering = jnp.zeros((length, value_width), F32)
        for d in range(1, n_sp):
            slot = (n_sp - d if back else d) - 1
            valid = (s + d < n_sp) if back else (s - d >= 0)
            aux = auxes[slot]
            facing = aux[2:3] if back else aux[3:4]
            joined = jnp.where(facing == edge, jnp.where(valid, 1.0, 0.0), 0.0)
            state = states[slot, back * DK : (back + 1) * DK]
            state = jnp.where(own, jnp.concatenate([state] * heads, axis=0), jnp.zeros((), BF16))
            entering = entering + dot((query * jnp.where(joined > 0.0, reach, 0.0)).astype(BF16), state)
            reach = reach * aux[back : back + 1]
        attended = attended + jnp.where(doc == edge, entering, 0.0)
    group = (iota((value_width, value_width), 0) // DV) == (iota((value_width, value_width), 1) // DV)
    mean_square = dot(attended * attended, jnp.where(group, 1.0 / DV, 0.0), precision=HIGH)
    u = outgate_ref[...].astype(F32)
    mixed = attended * lax.rsqrt(mean_square + EPS) * headgain_ref[...] * (u / (1.0 + jnp.exp(-u)))
    mixed = mixed.astype(BF16)
    for i in range(n_tp):
        sendbuf[i] = dot(mixed, outweight_ref[:, i * own_width : (i + 1) * own_width]).astype(BF16)

    def norm(stream, kind):
        ones = jnp.ones((8, own_width), F32)
        sums = dot(ones, stream, ((1,), (1,)), HIGH)
        squares = dot(ones, stream * stream, ((1,), (1,)), HIGH)
        moments[kind] = jnp.where(iota((8, length), 0) == 0, sums, squares)
        copies = to_tp(2 + kind, lambda to: moments.at[kind], lambda d: moments_in.at[kind, d - 1])
        for copy in copies:
            copy.wait_recv()
        total = moments[kind]
        for d in range(1, n_tp):
            total = total + moments_in[kind, d - 1]
        eye = jnp.where(iota((length, length), 0) == iota((length, length), 1), 1.0, 0.0)
        total = dot(eye, total, ((1,), (1,)), HIGH) / full_width
        middle = total[:, 0:1]
        spread = total[:, 1:2] - middle * middle
        return (stream - middle) * lax.rsqrt(spread + EPS) * gain_ref[kind, t] + bias_ref[kind, t]

    copies = to_tp(0, lambda to: sendbuf.at[to], lambda d: landed.at[d - 1])
    pump(1)
    for copy in copies:
        copy.wait_recv()
    stream = sendbuf[t].astype(F32)
    for d in range(1, n_tp):
        stream = stream + landed[d - 1].astype(F32)
    settled = norm(residual_ref[...].astype(F32) + stream, 0)
    features[t] = settled.astype(BF16)
    copies = to_tp(1, lambda to: features.at[t], lambda d: features.at[t])
    pump(2)
    for copy in copies:
        copy.wait_recv()

    pump(len(events) - cursor[0] - 1)
    own_copies[0].wait()
    own_copies[1].wait()
    for k in range(1, n_sp):
        for p in range(2):
            finish_across(k, p)
    depth = gate_hbm.shape[0]

    def project(weights):
        out = None
        for i in range(n_tp):
            block = own_width // depth
            term = dot(features[i], weights[i * block : (i + 1) * block].reshape(own_width, weights.shape[2]))
            out = term if out is None else out + term
        return out

    gate = project(gate_all)
    inner = (gate / (1.0 + jnp.exp(-gate)) * project(up_all)).astype(BF16)

    pump(1)
    own_copies[2].wait()
    for k in range(1, n_sp):
        finish_across(k, 2)
    piece = down_hbm.shape[1]
    for i in range(n_sp):
        owner, at = (i * piece) // own_width, (i * piece) % own_width
        sendbuf2[owner, :, at : at + piece] = dot(inner, down_all[i]).astype(BF16)
    copies = to_tp(4, lambda to: sendbuf2.at[to], lambda d: landed2.at[d - 1])
    for copy in copies:
        copy.wait_recv()
    down = sendbuf2[t].astype(F32)
    for d in range(1, n_tp):
        down = down + landed2[d - 1].astype(F32)
    result_ref[...] = norm(settled + 0.5 * down, 1).astype(BF16)

    for copy in sent:
        copy.wait_send()
    for p in range(3):
        for way in range(2):
            step = 1 if way == 0 else -1
            for k in range(n_sp - 1):

                @pl.when(inside(s + step) & inside(s - step * k))
                def _(p=p, way=way, k=k, step=step):
                    along(p, way, k, s - step * k).wait_send()

            for k in range(1, n_sp):

                @pl.when(inside(s - step * k))
                def _(p=p, way=way, k=k, step=step):
                    for d in range(1, n_grp):
                        across(p, way, k, s - step * k, d).wait_send()


def on_device(
    sizes,
    queries,
    key_rows,
    value_rows,
    out_gate,
    log_decay,
    doc_ids,
    head_gain,
    out_weight,
    residual,
    norm_gain,
    norm_bias,
    gate_weight,
    up_weight,
    down_weight,
):
    n_grp, n_sp, n_tp = sizes
    length, width = queries.shape
    value_width = value_rows.shape[1]
    own_width = residual.shape[1]
    heads = width // DK
    doc = doc_ids.astype(F32)
    doc_column, doc_row = doc[:, None], doc[None, :]
    local, qf, qb, state, aux = pl.pallas_call(
        attend_kernel,
        out_shape=(
            jax.ShapeDtypeStruct((length, value_width), F32),
            jax.ShapeDtypeStruct((length, width), F32),
            jax.ShapeDtypeStruct((length, width), F32),
            jax.ShapeDtypeStruct((2 * DK, value_width), BF16),
            jax.ShapeDtypeStruct((8, width), F32),
        ),
        scratch_shapes=[VMEM((heads * length, length), F32)],
        compiler_params=pltpu.CompilerParams(vmem_limit_bytes=24 * 2**20),
        name="attend",
    )(queries, key_rows, value_rows, log_decay, doc_column, doc_row)

    vm = pl.BlockSpec(memory_space=VMEM)
    hbm = pl.BlockSpec(memory_space=pl.ANY)
    dma = pltpu.SemaphoreType.DMA
    hops = max(n_grp - 1, 1)
    return pl.pallas_call(
        functools.partial(layer_kernel, sizes),
        out_shape=jax.ShapeDtypeStruct((length, own_width), BF16),
        in_specs=[vm] * 12 + [hbm] * 3,
        out_specs=vm,
        scratch_shapes=[
            VMEM((n_sp,) + gate_weight.shape, BF16),
            VMEM((n_sp,) + up_weight.shape, BF16),
            VMEM((n_sp,) + down_weight.shape, BF16),
            VMEM((n_sp - 1, 2 * DK, value_width), BF16),
            VMEM((n_sp - 1, 8, width), F32),
            VMEM((n_tp, length, own_width), BF16),
            VMEM((n_tp - 1, length, own_width), BF16),
            VMEM((n_tp, length, own_width), BF16),
            VMEM((n_tp - 1, length, own_width), BF16),
            VMEM((n_tp, length, own_width), BF16),
            VMEM((2, 8, length), F32),
            VMEM((2, n_tp - 1, 8, length), F32),
            dma((2, n_sp - 1)),
            dma((2, n_sp - 1)),
            dma((3, 2, n_sp)),
            dma((3, 2, n_sp)),
            dma((3, 2, n_sp, hops)),
            dma((3, 2, n_sp, hops)),
            dma((5, n_tp - 1)),
            dma((5, n_tp - 1)),
            dma((3,)),
        ],
        compiler_params=pltpu.CompilerParams(
            collective_id=0, has_side_effects=True, vmem_limit_bytes=48 * 2**20
        ),
        name="layer",
    )(
        local,
        qf,
        qb,
        state,
        aux,
        doc_column,
        out_gate,
        head_gain[None, :],
        out_weight,
        residual,
        norm_gain.reshape(2, n_tp, 1, own_width),
        norm_bias.reshape(2, n_tp, 1, own_width),
        gate_weight,
        up_weight,
        down_weight,
    )


def solution(mesh):
    sizes = tuple(mesh.shape[axis] for axis in ("grp", "sp", "tp"))
    in_specs = (
        P(("grp", "sp"), "tp"),
        P(("grp", "sp"), "tp"),
        P(("grp", "sp"), "tp"),
        P(("grp", "sp"), "tp"),
        P(None, ("grp", "sp"), "tp"),
        P(("grp", "sp")),
        P("tp"),
        P("tp", None),
        P(("grp", "sp"), "tp"),
        P(),
        P(),
        P("sp", "tp"),
        P("sp", "tp"),
        P("tp", "sp"),
    )
    return jax.shard_map(
        functools.partial(on_device, sizes),
        mesh=mesh,
        in_specs=in_specs,
        out_specs=P(("grp", "sp"), "tp"),
        check_vma=False,
    )
```

```python
import functools

import jax
import jax.numpy as jnp
from jax import lax
from jax.experimental import pallas as pl
from jax.experimental.pallas import tpu as pltpu
from jax.sharding import PartitionSpec as P

DK = 32
DV = 64
EPS = 1e-06
F32 = jnp.float32
BF16 = jnp.bfloat16
HIGH = lax.Precision.HIGHEST
MESH = pl.DeviceIdType.MESH
VMEM = pltpu.VMEM
PIECES = ((0, 0, 2), (0, 1, 2), (1, 0, 1), (2, 0, 2), (2, 1, 2))


def dot(a, b, dims=((1,), (0,)), precision=None):
    return lax.dot_general(a, b, (dims, ((), ())), precision=precision, preferred_element_type=F32)


def iota(shape, axis):
    return lax.broadcasted_iota(jnp.int32, shape, axis)


def attend(q_ref, k_ref, v_ref, decay_ref, doc, doc_row, out_ref, qf_ref, qb_ref, state_ref, aux_ref, acc):
    length, width = q_ref.shape
    heads = width // DK
    q = q_ref[...].astype(F32) * DK**-0.5
    k = k_ref[...].astype(F32)
    v = v_ref[...]
    row = iota((length, width), 0)
    far = iota((length, length), 0) ^ iota((length, length), 1)
    lane_head = (iota((length, 2 * width), 1) % width) // DK
    zero = jnp.zeros((length, width), F32)

    def scores(left, right):
        left, right = left.astype(BF16), right.astype(BF16)
        lanes = lane_head[:, : left.shape[1]]
        stacked = jnp.concatenate([jnp.where(lanes == h, left, jnp.zeros_like(left)) for h in range(heads)], axis=0)
        return dot(stacked, right, ((1,), (1,)))

    acc[...] = 2.0 * scores(q, k)
    total_f, total_b = decay_ref[0], decay_ref[1]
    prefix_f, suffix_b = total_f, total_b
    suffix_f, prefix_b = zero, zero
    span = 1
    while span < length:
        upper = (row & span) != 0
        left = jnp.concatenate(
            [jnp.where(upper, q * jnp.exp(prefix_f), 0.0), jnp.where(upper, 0.0, q * jnp.exp(suffix_b))], axis=1
        )
        right = jnp.concatenate(
            [jnp.where(upper, 0.0, k * jnp.exp(suffix_f)), jnp.where(upper, k * jnp.exp(prefix_b), 0.0)], axis=1
        )
        product = scores(left, right)
        for h in range(heads):
            rows = slice(h * length, (h + 1) * length)
            acc[rows] = jnp.where(far >= span, product[rows], acc[rows])

        def other(x):
            return jnp.where(upper, pltpu.roll(x, span, 0), pltpu.roll(x, length - span, 0))

        beside_f, beside_b = other(total_f), other(total_b)
        prefix_f = prefix_f + jnp.where(upper, beside_f, 0.0)
        suffix_f = suffix_f + jnp.where(upper, 0.0, beside_f)
        suffix_b = suffix_b + jnp.where(upper, 0.0, beside_b)
        prefix_b = prefix_b + jnp.where(upper, beside_b, 0.0)
        total_f, total_b = total_f + beside_f, total_b + beside_b
        span *= 2

    same = doc == doc_row
    value_head = iota((length, v.shape[1]), 1) // DV
    result = jnp.zeros((length, v.shape[1]), F32)
    for h in range(heads):
        weights = jnp.where(same, acc[h * length : (h + 1) * length], 0.0).astype(BF16)
        result = jnp.where(value_head == h, dot(weights, v), result)
    out_ref[...] = result
    qf_ref[...] = q * jnp.exp(prefix_f)
    qb_ref[...] = q * jnp.exp(suffix_b)

    first, last = doc[:1], doc[length - 1 :]
    own = (iota((width, v.shape[1]), 0) // DK) == (iota((width, v.shape[1]), 1) // DV)
    for i, (reach, edge) in enumerate(((suffix_f, last), (prefix_b, first))):
        kept = jnp.where(doc == edge, k * jnp.exp(reach), 0.0).astype(BF16)
        state = jnp.where(own, dot(kept, v, ((0,), (0,))), 0.0)
        packed = state[:DK]
        for h in range(1, heads):
            packed = packed + state[h * DK : (h + 1) * DK]
        state_ref[i * DK : (i + 1) * DK] = packed.astype(BF16)
    edge_row = iota((8, width), 0)
    aux = jnp.where(edge_row == 0, jnp.exp(total_f[:8]), jnp.exp(total_b[:8]))
    aux = jnp.where(edge_row == 2, first, aux)
    aux_ref[...] = jnp.where(edge_row == 3, last, aux)


def layer_kernel(sizes, *refs):
    (
        q_hbm, k_hbm, v_hbm, outgate_hbm, decay_hbm, docrow_hbm, headgain_hbm, outweight_hbm, residual_hbm,
        gain_hbm, bias_hbm, gate_hbm, up_hbm, down_hbm, result_ref,
        q_ref, k_ref, v_ref, outgate_ref, decay_ref, docrow_ref, headgain_ref, outweight_ref, residual_ref,
        gain_ref, bias_ref, local_ref, qf_ref, qb_ref, state_ref, aux_ref, acc, inner_ref,
        gate_all, up_all, down_all, states, auxes, sendbuf, landed, sendbuf2, landed2, features, moments,
        moments_in, small_send, small_recv, z_send, z_recv, y_send, y_recv, tp_send, tp_recv, local_sem, in_sem,
    ) = refs
    n_grp, n_sp, n_tp = sizes
    g, s, t = lax.axis_index("grp"), lax.axis_index("sp"), lax.axis_index("tp")
    length = q_hbm.shape[0]
    own_width = residual_hbm.shape[1]
    full_width = own_width * n_tp

    def around(axis, me, n, d):
        return {axis: lax.rem(me + d, n)}

    mine = pl.ds(pl.multiple_of(t * own_width, own_width), own_width)
    loads = []
    for i, (src, dst) in enumerate(
        (
            (decay_hbm, decay_ref),
            (q_hbm, q_ref),
            (k_hbm, k_ref),
            (docrow_hbm, docrow_ref),
            (v_hbm, v_ref),
            (outgate_hbm, outgate_ref),
            (headgain_hbm, headgain_ref),
            (outweight_hbm, outweight_ref),
            (residual_hbm, residual_ref),
            (gain_hbm.at[:, mine], gain_ref),
            (bias_hbm.at[:, mine], bias_ref),
        )
    ):
        loads.append(pltpu.make_async_copy(src, dst, in_sem.at[i]))
        loads[-1].start()

    barrier = pltpu.get_barrier_semaphore()
    for axis, me, n in (("grp", g, n_grp), ("sp", s, n_sp), ("tp", t, n_tp)):
        for d in range(1, n):
            pl.semaphore_signal(barrier, inc=1, device_id=around(axis, me, n, d), device_id_type=MESH)
    pl.semaphore_wait(barrier, n_grp + n_sp + n_tp - 3)

    sent = []

    def remote(src, dst, ssem, rsem, to):
        return pltpu.make_async_remote_copy(
            src_ref=src, dst_ref=dst, send_sem=ssem, recv_sem=rsem, device_id=to, device_id_type=MESH
        )

    whole = ((gate_hbm, gate_all), (up_hbm, up_all), (down_hbm, down_all))
    pieces = PIECES
    n_up = sum(1 for which, _, _ in pieces if which < 2)

    def rows_of(p, which):
        weight, share, shares = pieces[p]
        src, dst = whole[weight]
        rows = src.shape[0] // (n_grp * shares)
        return src, dst, pl.ds(pl.multiple_of((which * shares + share) * rows, rows), rows)

    def part(p, origin, which):
        _, dst, rows = rows_of(p, which)
        return dst.at[origin, rows, :]

    def own_part(p):
        src, _, rows = rows_of(p, g)
        return src.at[rows, :]

    def along(p, way, k, origin):
        step = 1 if way == 0 else -1
        src = own_part(p) if k == 0 else part(p, origin, g)
        return remote(
            src, part(p, origin, g), z_send.at[p, way, k], z_recv.at[p, way, k], {"sp": lax.rem(s + step + n_sp, n_sp)}
        )

    def across(p, way, k, origin, d):
        return remote(
            part(p, origin, g), part(p, origin, g), y_send.at[p, way, k, d - 1], y_recv.at[p, way, k, d - 1],
            around("grp", g, n_grp, d),
        )

    def inside(x):
        return (x >= 0) & (x < n_sp)

    def start_own(p):
        for way in range(2):
            step = 1 if way == 0 else -1

            @pl.when(inside(s + step))
            def _(way=way):
                along(p, way, 0, s).start()

    own_copies = []
    for p in range(3):
        own_copies.append(pltpu.make_async_copy(whole[p][0], whole[p][1].at[s], local_sem.at[p]))

    def relay(k, p):
        for way in range(2):
            step = 1 if way == 0 else -1
            origin = s - step * k

            @pl.when(inside(origin))
            def _(way=way, step=step, origin=origin):
                along(p, way, k - 1, origin).wait_recv()
                if k < n_sp - 1:

                    @pl.when(inside(s + step))
                    def _():
                        along(p, way, k, origin).start()

                for d in range(1, n_grp):
                    across(p, way, k, origin, d).start()

    def finish_across(k, p):
        for way in range(2):
            origin = s - (1 if way == 0 else -1) * k

            @pl.when(inside(origin))
            def _(way=way, origin=origin):
                for d in range(1, n_grp):
                    arrived = part(p, origin, lax.rem(g - d + n_grp, n_grp))
                    sems = (y_send.at[p, way, k, d - 1], y_recv.at[p, way, k, d - 1])
                    remote(arrived, arrived, *sems, around("grp", g, n_grp, d)).wait_recv()

    events = [(k, p) for k in range(1, n_sp) for p in range(len(pieces))]
    cursor = [0]

    def pump(count):
        for k, p in events[cursor[0] : cursor[0] + count]:
            relay(k, p)
        cursor[0] += count

    def to_tp(kind, src_of, dst_of):
        copies = []
        for d in range(1, n_tp):
            to = lax.rem(t + d, n_tp)
            copy = remote(
                src_of(to), dst_of(d), tp_send.at[kind, d - 1], tp_recv.at[kind, d - 1], {"tp": to}
            )
            copy.start()
            copies.append(copy)
        sent.extend(copies)
        return copies

    start_own(0)
    for load in loads[:5]:
        load.wait()
    doc_row = docrow_ref[...]
    eye = iota((length, length), 0) == iota((length, length), 1)
    doc = jnp.sum(jnp.where(eye, doc_row, 0), axis=1, keepdims=True).astype(F32)
    attend(
        q_ref, k_ref, v_ref, decay_ref, doc, doc_row.astype(F32), local_ref, qf_ref, qb_ref, state_ref, aux_ref, acc
    )
    small = []
    for d in range(1, n_sp):
        to = around("sp", s, n_sp, d)
        for j, (src, dst) in enumerate(((state_ref, states), (aux_ref, auxes))):
            copy = remote(src, dst.at[d - 1], small_send.at[j, d - 1], small_recv.at[j, d - 1], to)
            copy.start()
            small.append(copy)

    for p in range(1, len(pieces)):
        start_own(p)
    for copy in own_copies:
        copy.start()
    for load in loads[5:]:
        load.wait()
    pump(1)

    for copy in small:
        copy.wait_recv()
    sent.extend(small)
    first, last = doc[:1], doc[length - 1 :]
    width = qf_ref.shape[1]
    heads = width // DK
    value_width = local_ref.shape[1]
    own = (iota((width, value_width), 0) // DK) == (iota((width, value_width), 1) // DV)
    attended = local_ref[...]
    for back in range(2):
        query = (qb_ref if back else qf_ref)[...]
        edge = last if back else first
        reach = jnp.ones((1, width), F32)
        entering = jnp.zeros((length, value_width), F32)
        for d in range(1, n_sp):
            slot = (n_sp - d if back else d) - 1
            valid = (s + d < n_sp) if back else (s - d >= 0)
            aux = auxes[slot]
            facing = aux[2:3] if back else aux[3:4]
            joined = jnp.where(facing == edge, jnp.where(valid, 1.0, 0.0), 0.0)
            state = states[slot, back * DK : (back + 1) * DK]
            state = jnp.where(own, jnp.concatenate([state] * heads, axis=0), jnp.zeros((), BF16))
            entering = entering + dot((query * jnp.where(joined > 0.0, reach, 0.0)).astype(BF16), state)
            reach = reach * aux[back : back + 1]
        attended = attended + jnp.where(doc == edge, entering, 0.0)
    group = (iota((value_width, value_width), 0) // DV) == (iota((value_width, value_width), 1) // DV)
    mean_square = dot(attended * attended, jnp.where(group, 1.0 / DV, 0.0), precision=HIGH)
    u = outgate_ref[...].astype(F32)
    mixed = attended * lax.rsqrt(mean_square + EPS) * headgain_ref[...] * (u / (1.0 + jnp.exp(-u)))
    mixed = mixed.astype(BF16)
    for i in range(n_tp):
        sendbuf[i] = dot(mixed, outweight_ref[:, i * own_width : (i + 1) * own_width]).astype(BF16)

    def norm(stream, kind):
        ones = jnp.ones((8, own_width), F32)
        sums = dot(ones, stream, ((1,), (1,)), HIGH)
        squares = dot(ones, stream * stream, ((1,), (1,)), HIGH)
        moments[kind] = jnp.where(iota((8, length), 0) == 0, sums, squares)
        copies = to_tp(2 + kind, lambda to: moments.at[kind], lambda d: moments_in.at[kind, d - 1])
        for copy in copies:
            copy.wait_recv()
        total = moments[kind]
        for d in range(1, n_tp):
            total = total + moments_in[kind, d - 1]
        total = dot(jnp.where(eye, 1.0, 0.0), total, ((1,), (1,)), HIGH) / full_width
        middle = total[:, 0:1]
        spread = total[:, 1:2] - middle * middle
        return (stream - middle) * lax.rsqrt(spread + EPS) * gain_ref[kind : kind + 1] + bias_ref[kind : kind + 1]

    copies = to_tp(0, lambda to: sendbuf.at[to], lambda d: landed.at[d - 1])
    pump(2)
    for copy in copies:
        copy.wait_recv()
    pump(1)
    stream = sendbuf[t].astype(F32)
    for d in range(1, n_tp):
        stream = stream + landed[d - 1].astype(F32)
    settled = norm(residual_ref[...].astype(F32) + stream, 0)
    features[t] = settled.astype(BF16)
    copies = to_tp(1, lambda to: features.at[t], lambda d: features.at[t])
    pump(2)
    for copy in copies:
        copy.wait_recv()

    pump(len(events) - cursor[0])
    for copy in own_copies:
        copy.wait()
    for k in range(1, n_sp):
        for p in range(n_up):
            finish_across(k, p)
    depth = gate_hbm.shape[0]

    def project(weights):
        out = None
        for i in range(n_tp):
            block = own_width // depth
            term = dot(features[i], weights[i * block : (i + 1) * block].reshape(own_width, weights.shape[2]))
            out = term if out is None else out + term
        return out

    gate = project(gate_all)
    inner_ref[...] = (gate / (1.0 + jnp.exp(-gate)) * project(up_all)).astype(BF16)

    piece = down_hbm.shape[1]
    if piece == own_width:
        def deliver(owner):
            d = lax.rem(owner - t + n_tp, n_tp)
            at = jnp.maximum(d - 1, 0)
            return remote(
                sendbuf2.at[owner], landed2.at[at], tp_send.at[4, at], tp_recv.at[4, at], {"tp": owner}
            )

        def one_block(origin):
            sendbuf2[origin] = dot(inner_ref[...], down_all[origin]).astype(BF16)

            @pl.when(origin != t)
            def _():
                deliver(origin).start()

        one_block(s)
        for k in range(1, n_sp):
            for p in range(n_up, len(pieces)):
                finish_across(k, p)
            for way in range(2):
                origin = s - (1 if way == 0 else -1) * k

                @pl.when(inside(origin))
                def _(origin=origin):
                    one_block(origin)

        copies = [
            remote(
                sendbuf2.at[lax.rem(t + d, n_tp)], landed2.at[d - 1], tp_send.at[4, d - 1], tp_recv.at[4, d - 1],
                {"tp": lax.rem(t + d, n_tp)},
            )
            for d in range(1, n_tp)
        ]
        sent.extend(copies)
    else:
        for k in range(1, n_sp):
            for p in range(n_up, len(pieces)):
                finish_across(k, p)
        for i in range(n_sp):
            owner, at = (i * piece) // own_width, (i * piece) % own_width
            sendbuf2[owner, :, at : at + piece] = dot(inner_ref[...], down_all[i]).astype(BF16)
        copies = to_tp(4, lambda to: sendbuf2.at[to], lambda d: landed2.at[d - 1])
    for copy in copies:
        copy.wait_recv()
    down = sendbuf2[t].astype(F32)
    for d in range(1, n_tp):
        down = down + landed2[d - 1].astype(F32)
    result_ref[...] = norm(settled + 0.5 * down, 1).astype(BF16)

    for copy in sent:
        copy.wait_send()
    for p in range(len(pieces)):
        for way in range(2):
            step = 1 if way == 0 else -1
            for k in range(n_sp - 1):

                @pl.when(inside(s + step) & inside(s - step * k))
                def _(p=p, way=way, k=k, step=step):
                    along(p, way, k, s - step * k).wait_send()

            for k in range(1, n_sp):

                @pl.when(inside(s - step * k))
                def _(p=p, way=way, k=k, step=step):
                    for d in range(1, n_grp):
                        across(p, way, k, s - step * k, d).wait_send()


def on_device(
    sizes,
    queries,
    key_rows,
    value_rows,
    out_gate,
    log_decay,
    doc_ids,
    head_gain,
    out_weight,
    residual,
    norm_gain,
    norm_bias,
    gate_weight,
    up_weight,
    down_weight,
):
    n_grp, n_sp, n_tp = sizes
    length, width = queries.shape
    value_width = value_rows.shape[1]
    own_width = residual.shape[1]
    heads = width // DK
    vm = pl.BlockSpec(memory_space=VMEM)
    hbm = pl.BlockSpec(memory_space=pl.ANY)
    dma = pltpu.SemaphoreType.DMA
    hops = max(n_grp - 1, 1)
    return pl.pallas_call(
        functools.partial(layer_kernel, sizes),
        out_shape=jax.ShapeDtypeStruct((length, own_width), BF16),
        in_specs=[hbm] * 14,
        out_specs=vm,
        scratch_shapes=[
            VMEM((length, width), BF16),
            VMEM((length, width), BF16),
            VMEM((length, value_width), BF16),
            VMEM((length, value_width), BF16),
            VMEM((2, length, width), F32),
            VMEM((1, length), jnp.int32),
            VMEM((1, value_width), F32),
            VMEM(out_weight.shape, BF16),
            VMEM((length, own_width), BF16),
            VMEM((2, own_width), F32),
            VMEM((2, own_width), F32),
            VMEM((length, value_width), F32),
            VMEM((length, width), F32),
            VMEM((length, width), F32),
            VMEM((2 * DK, value_width), BF16),
            VMEM((8, width), F32),
            VMEM((heads * length, length), F32),
            VMEM((length, gate_weight.shape[1]), BF16),
            VMEM((n_sp,) + gate_weight.shape, BF16),
            VMEM((n_sp,) + up_weight.shape, BF16),
            VMEM((n_sp,) + down_weight.shape, BF16),
            VMEM((n_sp - 1, 2 * DK, value_width), BF16),
            VMEM((n_sp - 1, 8, width), F32),
            VMEM((n_tp, length, own_width), BF16),
            VMEM((n_tp - 1, length, own_width), BF16),
            VMEM((n_tp, length, own_width), BF16),
            VMEM((n_tp - 1, length, own_width), BF16),
            VMEM((n_tp, length, own_width), BF16),
            VMEM((2, 8, length), F32),
            VMEM((2, n_tp - 1, 8, length), F32),
            dma((2, n_sp - 1)),
            dma((2, n_sp - 1)),
            dma((len(PIECES), 2, n_sp)),
            dma((len(PIECES), 2, n_sp)),
            dma((len(PIECES), 2, n_sp, hops)),
            dma((len(PIECES), 2, n_sp, hops)),
            dma((5, n_tp - 1)),
            dma((5, n_tp - 1)),
            dma((3,)),
            dma((11,)),
        ],
        compiler_params=pltpu.CompilerParams(
            collective_id=0, has_side_effects=True, vmem_limit_bytes=60 * 2**20
        ),
        name="layer",
    )(
        queries,
        key_rows,
        value_rows,
        out_gate,
        log_decay,
        doc_ids[None, :],
        head_gain[None, :],
        out_weight,
        residual,
        norm_gain,
        norm_bias,
        gate_weight,
        up_weight,
        down_weight,
    )


def solution(mesh):
    sizes = tuple(mesh.shape[axis] for axis in ("grp", "sp", "tp"))
    in_specs = (
        P(("grp", "sp"), "tp"),
        P(("grp", "sp"), "tp"),
        P(("grp", "sp"), "tp"),
        P(("grp", "sp"), "tp"),
        P(None, ("grp", "sp"), "tp"),
        P(("grp", "sp")),
        P("tp"),
        P("tp", None),
        P(("grp", "sp"), "tp"),
        P(),
        P(),
        P("sp", "tp"),
        P("sp", "tp"),
        P("tp", "sp"),
    )
    return jax.shard_map(
        functools.partial(on_device, sizes),
        mesh=mesh,
        in_specs=in_specs,
        out_specs=P(("grp", "sp"), "tp"),
        check_vma=False,
    )
```

```python
import functools

import jax
import jax.numpy as jnp
from jax import lax
from jax.experimental import pallas as pl
from jax.experimental.pallas import tpu as pltpu
from jax.sharding import PartitionSpec as P

DK = 32
DV = 64
EPS = 1e-06
F32 = jnp.float32
BF16 = jnp.bfloat16
HIGH = lax.Precision.HIGHEST
MESH = pl.DeviceIdType.MESH
VMEM = pltpu.VMEM
PIECES = ((0, 0, 2), (0, 1, 2), (1, 0, 1), (2, 0, 2), (2, 1, 2))


def dot(a, b, dims=((1,), (0,)), precision=None):
    return lax.dot_general(a, b, (dims, ((), ())), precision=precision, preferred_element_type=F32)


def iota(shape, axis):
    return lax.broadcasted_iota(jnp.int32, shape, axis)


def attend(q_ref, k_ref, v_ref, decay_ref, doc, doc_row, out_ref, qf_ref, qb_ref, state_ref, aux_ref, acc):
    length, width = q_ref.shape
    heads = width // DK
    q = q_ref[...].astype(F32) * DK**-0.5
    k = k_ref[...].astype(F32)
    v = v_ref[...]
    row = iota((length, width), 0)
    far = iota((length, length), 0) ^ iota((length, length), 1)
    lane_head = (iota((length, 2 * width), 1) % width) // DK
    zero = jnp.zeros((length, width), F32)

    def scores(left, right):
        left, right = left.astype(BF16), right.astype(BF16)
        lanes = lane_head[:, : left.shape[1]]
        stacked = jnp.concatenate([jnp.where(lanes == h, left, jnp.zeros_like(left)) for h in range(heads)], axis=0)
        return dot(stacked, right, ((1,), (1,)))

    acc[...] = 2.0 * scores(q, k)
    total_f, total_b = decay_ref[0], decay_ref[1]
    prefix_f, suffix_b = total_f, total_b
    suffix_f, prefix_b = zero, zero
    span = 1
    while span < length:
        upper = (row & span) != 0
        left = jnp.concatenate(
            [jnp.where(upper, q * jnp.exp(prefix_f), 0.0), jnp.where(upper, 0.0, q * jnp.exp(suffix_b))], axis=1
        )
        right = jnp.concatenate(
            [jnp.where(upper, 0.0, k * jnp.exp(suffix_f)), jnp.where(upper, k * jnp.exp(prefix_b), 0.0)], axis=1
        )
        product = scores(left, right)
        for h in range(heads):
            rows = slice(h * length, (h + 1) * length)
            acc[rows] = jnp.where(far >= span, product[rows], acc[rows])

        def other(x):
            return jnp.where(upper, pltpu.roll(x, span, 0), pltpu.roll(x, length - span, 0))

        beside_f, beside_b = other(total_f), other(total_b)
        prefix_f = prefix_f + jnp.where(upper, beside_f, 0.0)
        suffix_f = suffix_f + jnp.where(upper, 0.0, beside_f)
        suffix_b = suffix_b + jnp.where(upper, 0.0, beside_b)
        prefix_b = prefix_b + jnp.where(upper, beside_b, 0.0)
        total_f, total_b = total_f + beside_f, total_b + beside_b
        span *= 2

    same = doc == doc_row
    value_head = iota((length, v.shape[1]), 1) // DV
    result = jnp.zeros((length, v.shape[1]), F32)
    for h in range(heads):
        weights = jnp.where(same, acc[h * length : (h + 1) * length], 0.0).astype(BF16)
        result = jnp.where(value_head == h, dot(weights, v), result)
    out_ref[...] = result
    qf_ref[...] = q * jnp.exp(prefix_f)
    qb_ref[...] = q * jnp.exp(suffix_b)

    first, last = doc[:1], doc[length - 1 :]
    own = (iota((width, v.shape[1]), 0) // DK) == (iota((width, v.shape[1]), 1) // DV)
    for i, (reach, edge) in enumerate(((suffix_f, last), (prefix_b, first))):
        kept = jnp.where(doc == edge, k * jnp.exp(reach), 0.0).astype(BF16)
        state = jnp.where(own, dot(kept, v, ((0,), (0,))), 0.0)
        packed = state[:DK]
        for h in range(1, heads):
            packed = packed + state[h * DK : (h + 1) * DK]
        state_ref[i * DK : (i + 1) * DK] = packed.astype(BF16)
    edge_row = iota((8, width), 0)
    aux = jnp.where(edge_row == 0, jnp.exp(total_f[:8]), jnp.exp(total_b[:8]))
    aux = jnp.where(edge_row == 2, first, aux)
    aux_ref[...] = jnp.where(edge_row == 3, last, aux)


def layer_kernel(sizes, *refs):
    (
        q_hbm, k_hbm, v_hbm, outgate_hbm, decay_hbm, docrow_hbm, headgain_hbm, outweight_hbm, residual_hbm,
        gain_hbm, bias_hbm, gate_hbm, up_hbm, down_hbm, result_ref,
        q_ref, k_ref, v_ref, outgate_ref, decay_ref, docrow_ref, headgain_ref, outweight_ref, residual_ref,
        gain_ref, bias_ref, local_ref, qf_ref, qb_ref, state_ref, aux_ref, acc, inner_ref,
        gate_all, up_all, down_all, states, auxes, sendbuf, landed, sendbuf2, landed2, features, moments,
        moments_in, small_send, small_recv, z_send, z_recv, y_send, y_recv, tp_send, tp_recv, local_sem, in_sem,
    ) = refs
    n_grp, n_sp, n_tp = sizes
    g, s, t = lax.axis_index("grp"), lax.axis_index("sp"), lax.axis_index("tp")
    length = q_hbm.shape[0]
    own_width = residual_hbm.shape[1]
    full_width = own_width * n_tp

    def around(axis, me, n, d):
        return {axis: lax.rem(me + d, n)}

    mine = pl.ds(pl.multiple_of(t * own_width, own_width), own_width)
    loads = []
    for i, (src, dst) in enumerate(
        (
            (decay_hbm, decay_ref),
            (q_hbm, q_ref),
            (k_hbm, k_ref),
            (docrow_hbm, docrow_ref),
            (v_hbm, v_ref),
            (outgate_hbm, outgate_ref),
            (headgain_hbm, headgain_ref),
            (outweight_hbm, outweight_ref),
            (residual_hbm, residual_ref),
            (gain_hbm.at[:, mine], gain_ref),
            (bias_hbm.at[:, mine], bias_ref),
        )
    ):
        loads.append(pltpu.make_async_copy(src, dst, in_sem.at[i]))
        loads[-1].start()

    barrier = pltpu.get_barrier_semaphore()
    for axis, me, n in (("grp", g, n_grp), ("sp", s, n_sp), ("tp", t, n_tp)):
        for d in range(1, n):
            pl.semaphore_signal(barrier, inc=1, device_id=around(axis, me, n, d), device_id_type=MESH)
    pl.semaphore_wait(barrier, n_grp + n_sp + n_tp - 3)

    sent = []

    def remote(src, dst, ssem, rsem, to):
        return pltpu.make_async_remote_copy(
            src_ref=src, dst_ref=dst, send_sem=ssem, recv_sem=rsem, device_id=to, device_id_type=MESH
        )

    whole = ((gate_hbm, gate_all), (up_hbm, up_all), (down_hbm, down_all))
    pieces = PIECES
    n_up = sum(1 for which, _, _ in pieces if which < 2)

    def rows_of(p, which):
        weight, share, shares = pieces[p]
        src, dst = whole[weight]
        rows = src.shape[0] // (n_grp * shares)
        return src, dst, pl.ds(pl.multiple_of((which * shares + share) * rows, rows), rows)

    def part(p, origin, which):
        _, dst, rows = rows_of(p, which)
        return dst.at[origin, rows, :]

    def own_part(p):
        src, _, rows = rows_of(p, g)
        return src.at[rows, :]

    def along(p, way, k, origin):
        step = 1 if way == 0 else -1
        src = own_part(p) if k == 0 else part(p, origin, g)
        return remote(
            src, part(p, origin, g), z_send.at[p, way, k], z_recv.at[p, way, k], {"sp": lax.rem(s + step + n_sp, n_sp)}
        )

    def across(p, way, k, origin, d):
        return remote(
            part(p, origin, g), part(p, origin, g), y_send.at[p, way, k, d - 1], y_recv.at[p, way, k, d - 1],
            around("grp", g, n_grp, d),
        )

    def inside(x):
        return (x >= 0) & (x < n_sp)

    def start_own(p):
        for way in range(2):
            step = 1 if way == 0 else -1

            @pl.when(inside(s + step))
            def _(way=way):
                along(p, way, 0, s).start()

    own_copies = []
    for p in range(3):
        own_copies.append(pltpu.make_async_copy(whole[p][0], whole[p][1].at[s], local_sem.at[p]))

    def relay(k, p):
        for way in range(2):
            step = 1 if way == 0 else -1
            origin = s - step * k

            @pl.when(inside(origin))
            def _(way=way, step=step, origin=origin):
                along(p, way, k - 1, origin).wait_recv()
                if k < n_sp - 1:

                    @pl.when(inside(s + step))
                    def _():
                        along(p, way, k, origin).start()

                for d in range(1, n_grp):
                    across(p, way, k, origin, d).start()

    def finish_across(k, p):
        for way in range(2):
            origin = s - (1 if way == 0 else -1) * k

            @pl.when(inside(origin))
            def _(way=way, origin=origin):
                for d in range(1, n_grp):
                    arrived = part(p, origin, lax.rem(g - d + n_grp, n_grp))
                    sems = (y_send.at[p, way, k, d - 1], y_recv.at[p, way, k, d - 1])
                    remote(arrived, arrived, *sems, around("grp", g, n_grp, d)).wait_recv()

    events = [(k, p) for k in range(1, n_sp) for p in range(len(pieces))]
    cursor = [0]

    def pump(count):
        for k, p in events[cursor[0] : cursor[0] + count]:
            relay(k, p)
        cursor[0] += count

    def to_tp(kind, src_of, dst_of):
        copies = []
        for d in range(1, n_tp):
            to = lax.rem(t + d, n_tp)
            copy = remote(
                src_of(to), dst_of(d), tp_send.at[kind, d - 1], tp_recv.at[kind, d - 1], {"tp": to}
            )
            copy.start()
            copies.append(copy)
        sent.extend(copies)
        return copies

    start_own(0)
    start_own(1)
    for load in loads[:5]:
        load.wait()
    doc_row = docrow_ref[...]
    eye = iota((length, length), 0) == iota((length, length), 1)
    doc = jnp.sum(jnp.where(eye, doc_row, 0), axis=1, keepdims=True).astype(F32)
    attend(
        q_ref, k_ref, v_ref, decay_ref, doc, doc_row.astype(F32), local_ref, qf_ref, qb_ref, state_ref, aux_ref, acc
    )
    small = []
    for d in range(1, n_sp):
        to = around("sp", s, n_sp, d)
        for j, (src, dst) in enumerate(((state_ref, states), (aux_ref, auxes))):
            copy = remote(src, dst.at[d - 1], small_send.at[j, d - 1], small_recv.at[j, d - 1], to)
            copy.start()
            small.append(copy)

    for p in range(2, len(pieces)):
        start_own(p)
    for copy in own_copies:
        copy.start()
    for load in loads[5:]:
        load.wait()
    pump(1)

    for copy in small:
        copy.wait_recv()
    sent.extend(small)
    first, last = doc[:1], doc[length - 1 :]
    width = qf_ref.shape[1]
    heads = width // DK
    value_width = local_ref.shape[1]
    own = (iota((width, value_width), 0) // DK) == (iota((width, value_width), 1) // DV)
    attended = local_ref[...]
    for back in range(2):
        query = (qb_ref if back else qf_ref)[...]
        edge = last if back else first
        reach = jnp.ones((1, width), F32)
        entering = jnp.zeros((length, value_width), F32)
        for d in range(1, n_sp):
            slot = (n_sp - d if back else d) - 1
            valid = (s + d < n_sp) if back else (s - d >= 0)
            aux = auxes[slot]
            facing = aux[2:3] if back else aux[3:4]
            joined = jnp.where(facing == edge, jnp.where(valid, 1.0, 0.0), 0.0)
            state = states[slot, back * DK : (back + 1) * DK]
            state = jnp.where(own, jnp.concatenate([state] * heads, axis=0), jnp.zeros((), BF16))
            entering = entering + dot((query * jnp.where(joined > 0.0, reach, 0.0)).astype(BF16), state)
            reach = reach * aux[back : back + 1]
        attended = attended + jnp.where(doc == edge, entering, 0.0)
    group = (iota((value_width, value_width), 0) // DV) == (iota((value_width, value_width), 1) // DV)
    mean_square = dot(attended * attended, jnp.where(group, 1.0 / DV, 0.0), precision=HIGH)
    u = outgate_ref[...].astype(F32)
    mixed = attended * lax.rsqrt(mean_square + EPS) * headgain_ref[...] * (u / (1.0 + jnp.exp(-u)))
    mixed = mixed.astype(BF16)
    for i in range(n_tp):
        sendbuf[i] = dot(mixed, outweight_ref[:, i * own_width : (i + 1) * own_width]).astype(BF16)

    def norm(stream, kind):
        def as_row(x):
            return jnp.sum(jnp.where(eye, jnp.sum(x, axis=1, keepdims=True), 0.0), axis=0, keepdims=True)

        moments[kind] = jnp.where(iota((8, length), 0) == 0, as_row(stream), as_row(stream * stream))
        copies = to_tp(2 + kind, lambda to: moments.at[kind], lambda d: moments_in.at[kind, d - 1])
        for copy in copies:
            copy.wait_recv()
        total = moments[kind]
        for d in range(1, n_tp):
            total = total + moments_in[kind, d - 1]
        total = total / full_width
        middle = jnp.sum(jnp.where(eye, total[0:1], 0.0), axis=1, keepdims=True)
        spread = jnp.sum(jnp.where(eye, total[1:2], 0.0), axis=1, keepdims=True) - middle * middle
        return (stream - middle) * lax.rsqrt(spread + EPS) * gain_ref[kind : kind + 1] + bias_ref[kind : kind + 1]

    copies = to_tp(0, lambda to: sendbuf.at[to], lambda d: landed.at[d - 1])
    pump(2)
    for copy in copies:
        copy.wait_recv()
    pump(1)
    stream = sendbuf[t].astype(F32)
    for d in range(1, n_tp):
        stream = stream + landed[d - 1].astype(F32)
    settled = norm(residual_ref[...].astype(F32) + stream, 0)
    features[t] = settled.astype(BF16)
    copies = to_tp(1, lambda to: features.at[t], lambda d: features.at[t])
    pump(2)
    for copy in copies:
        copy.wait_recv()

    pump(len(events) - cursor[0])
    for copy in own_copies:
        copy.wait()
    for k in range(1, n_sp):
        for p in range(n_up):
            finish_across(k, p)
    depth = gate_hbm.shape[0]

    def project(weights):
        out = None
        for i in range(n_tp):
            block = own_width // depth
            term = dot(features[i], weights[i * block : (i + 1) * block].reshape(own_width, weights.shape[2]))
            out = term if out is None else out + term
        return out

    gate = project(gate_all)
    inner_ref[...] = (gate / (1.0 + jnp.exp(-gate)) * project(up_all)).astype(BF16)

    piece = down_hbm.shape[1]
    if piece == own_width:
        def deliver(owner):
            d = lax.rem(owner - t + n_tp, n_tp)
            at = jnp.maximum(d - 1, 0)
            return remote(
                sendbuf2.at[owner], landed2.at[at], tp_send.at[4, at], tp_recv.at[4, at], {"tp": owner}
            )

        def one_block(origin):
            sendbuf2[origin] = dot(inner_ref[...], down_all[origin]).astype(BF16)

            @pl.when(origin != t)
            def _():
                deliver(origin).start()

        one_block(s)
        for k in range(1, n_sp):
            for p in range(n_up, len(pieces)):
                finish_across(k, p)
            for way in range(2):
                origin = s - (1 if way == 0 else -1) * k

                @pl.when(inside(origin))
                def _(origin=origin):
                    one_block(origin)

        copies = [
            remote(
                sendbuf2.at[lax.rem(t + d, n_tp)], landed2.at[d - 1], tp_send.at[4, d - 1], tp_recv.at[4, d - 1],
                {"tp": lax.rem(t + d, n_tp)},
            )
            for d in range(1, n_tp)
        ]
        sent.extend(copies)
    else:
        for k in range(1, n_sp):
            for p in range(n_up, len(pieces)):
                finish_across(k, p)
        for i in range(n_sp):
            owner, at = (i * piece) // own_width, (i * piece) % own_width
            sendbuf2[owner, :, at : at + piece] = dot(inner_ref[...], down_all[i]).astype(BF16)
        copies = to_tp(4, lambda to: sendbuf2.at[to], lambda d: landed2.at[d - 1])
    for copy in copies:
        copy.wait_recv()
    down = sendbuf2[t].astype(F32)
    for d in range(1, n_tp):
        down = down + landed2[d - 1].astype(F32)
    result_ref[...] = norm(settled + 0.5 * down, 1).astype(BF16)

    for copy in sent:
        copy.wait_send()
    for p in range(len(pieces)):
        for way in range(2):
            step = 1 if way == 0 else -1
            for k in range(n_sp - 1):

                @pl.when(inside(s + step) & inside(s - step * k))
                def _(p=p, way=way, k=k, step=step):
                    along(p, way, k, s - step * k).wait_send()

            for k in range(1, n_sp):

                @pl.when(inside(s - step * k))
                def _(p=p, way=way, k=k, step=step):
                    for d in range(1, n_grp):
                        across(p, way, k, s - step * k, d).wait_send()


def on_device(
    sizes,
    queries,
    key_rows,
    value_rows,
    out_gate,
    log_decay,
    doc_ids,
    head_gain,
    out_weight,
    residual,
    norm_gain,
    norm_bias,
    gate_weight,
    up_weight,
    down_weight,
):
    n_grp, n_sp, n_tp = sizes
    length, width = queries.shape
    value_width = value_rows.shape[1]
    own_width = residual.shape[1]
    heads = width // DK
    vm = pl.BlockSpec(memory_space=VMEM)
    hbm = pl.BlockSpec(memory_space=pl.ANY)
    dma = pltpu.SemaphoreType.DMA
    hops = max(n_grp - 1, 1)
    return pl.pallas_call(
        functools.partial(layer_kernel, sizes),
        out_shape=jax.ShapeDtypeStruct((length, own_width), BF16),
        in_specs=[hbm] * 14,
        out_specs=vm,
        scratch_shapes=[
            VMEM((length, width), BF16),
            VMEM((length, width), BF16),
            VMEM((length, value_width), BF16),
            VMEM((length, value_width), BF16),
            VMEM((2, length, width), F32),
            VMEM((1, length), jnp.int32),
            VMEM((1, value_width), F32),
            VMEM(out_weight.shape, BF16),
            VMEM((length, own_width), BF16),
            VMEM((2, own_width), F32),
            VMEM((2, own_width), F32),
            VMEM((length, value_width), F32),
            VMEM((length, width), F32),
            VMEM((length, width), F32),
            VMEM((2 * DK, value_width), BF16),
            VMEM((8, width), F32),
            VMEM((heads * length, length), F32),
            VMEM((length, gate_weight.shape[1]), BF16),
            VMEM((n_sp,) + gate_weight.shape, BF16),
            VMEM((n_sp,) + up_weight.shape, BF16),
            VMEM((n_sp,) + down_weight.shape, BF16),
            VMEM((n_sp - 1, 2 * DK, value_width), BF16),
            VMEM((n_sp - 1, 8, width), F32),
            VMEM((n_tp, length, own_width), BF16),
            VMEM((n_tp - 1, length, own_width), BF16),
            VMEM((n_tp, length, own_width), BF16),
            VMEM((n_tp - 1, length, own_width), BF16),
            VMEM((n_tp, length, own_width), BF16),
            VMEM((2, 8, length), F32),
            VMEM((2, n_tp - 1, 8, length), F32),
            dma((2, n_sp - 1)),
            dma((2, n_sp - 1)),
            dma((len(PIECES), 2, n_sp)),
            dma((len(PIECES), 2, n_sp)),
            dma((len(PIECES), 2, n_sp, hops)),
            dma((len(PIECES), 2, n_sp, hops)),
            dma((5, n_tp - 1)),
            dma((5, n_tp - 1)),
            dma((3,)),
            dma((11,)),
        ],
        compiler_params=pltpu.CompilerParams(
            collective_id=0, has_side_effects=True, vmem_limit_bytes=60 * 2**20
        ),
        name="layer",
    )(
        queries,
        key_rows,
        value_rows,
        out_gate,
        log_decay,
        doc_ids[None, :],
        head_gain[None, :],
        out_weight,
        residual,
        norm_gain,
        norm_bias,
        gate_weight,
        up_weight,
        down_weight,
    )


def solution(mesh):
    sizes = tuple(mesh.shape[axis] for axis in ("grp", "sp", "tp"))
    in_specs = (
        P(("grp", "sp"), "tp"),
        P(("grp", "sp"), "tp"),
        P(("grp", "sp"), "tp"),
        P(("grp", "sp"), "tp"),
        P(None, ("grp", "sp"), "tp"),
        P(("grp", "sp")),
        P("tp"),
        P("tp", None),
        P(("grp", "sp"), "tp"),
        P(),
        P(),
        P("sp", "tp"),
        P("sp", "tp"),
        P("tp", "sp"),
    )
    return jax.shard_map(
        functools.partial(on_device, sizes),
        mesh=mesh,
        in_specs=in_specs,
        out_specs=P(("grp", "sp"), "tp"),
        check_vma=False,
    )
```
